32 devices in a mesh: gr: 2 (over x), fs: 8 (over z, y), tp: 2 (over core).
Axes of the slice: x: 2, y: 2, z: 4, core: 2. Of those that a mesh axis runs over, the one named last changes fastest.
Arguments:
- tokens: bfloat16 [2816, 2048], P(('gr', 'fs')), may hold values from -6 to 6
- expert_ids: int32 [2816, 8], P(('gr', 'fs')), may hold values from 0 to 15, all different within a row; in each aligned block of 176 rows (0 to 175, 176 to 351, ...) at most 110 rows name the same one
- route_weight: float32 [2816, 8], P(('gr', 'fs')), may hold values from 0.05 to 1
- norm_gain: float32 [2048], P('tp'), may hold values from 0.1 to 1.9
- expert_gate: float32 [16, 512, 2048], P('gr', 'fs', 'tp'), may hold values from -0.125 to 0.125
- expert_up: float32 [16, 512, 2048], P('gr', 'fs', 'tp'), may hold values from -0.125 to 0.125
- expert_down: float32 [16, 512, 2048], P('gr', 'fs', 'tp'), may hold values from -0.25 to 0.25
- shared_gate: float32 [512, 2048], P('fs', 'tp'), may hold values from -0.125 to 0.125
- shared_up: float32 [512, 2048], P('fs', 'tp'), may hold values from -0.125 to 0.125
- shared_down: float32 [512, 2048], P('fs', 'tp'), may hold values from -0.25 to 0.25
Outputs:
- mixed: bfloat16 [2816, 2048], P(('gr', 'fs'), 'tp')
- new_gate: bfloat16 [2, 8, 512, 2048], P(None, 'fs', None, 'tp')
- new_up: bfloat16 [2, 8, 512, 2048], P(None, 'fs', None, 'tp')
- new_down: bfloat16 [2, 8, 512, 2048], P(None, 'fs', None, 'tp')
- new_shared_gate: bfloat16 [512, 2048], P(None, 'tp')
- new_shared_up: bfloat16 [512, 2048], P(None, 'tp')
- new_shared_down: bfloat16 [512, 2048], P(None, 'tp')
The draws below stay inside these ranges and needn't reach their ends.
Inputs may be any that keep to these rules, and one draw needn't show every extreme that they name: `expert_ids`: each row names 8 different experts; within each aligned block of 176 rows no expert is named by more than 110 rows, a bound that some block reaches.
All inputs are finite; a program needn't handle non-finite values.
Results may differ from the reference program's by a relative error of at most 0.022.
Values may be sent and summed in bfloat16 or wider, within the bound.
A program may use at most 128 MiB of HBM per device.

```python
import math
import jax
import jax.numpy as jnp
import numpy as np
from jax import lax

D = 2048
FF = 512
SHARED = 512
TOP = 8
TOK_DEV = 176
EXPERTS = 16
CAP = 110
TOKENS = 2816
N_GR = 2
N_FS = 8
N_TP = 2


def shard_levels(key, extent, shards, low, high):
    factor_of, own = 1.0, jax.random.fold_in(key, 6)
    for position, shards_of in shards:
        heights = jnp.exp(jax.random.uniform(jax.random.fold_in(own, position), (shards_of,), jnp.float32, low / len(shards), high / len(shards)))
        factor_of = factor_of * jnp.repeat(heights, extent[position] // shards_of).reshape([-1 if axis == position else 1 for axis in range(len(extent))])
    return factor_of


def routed_block(stream_key, own, number, rows, amount, top, limit, slope):
    sequence = jax.random.permutation(stream_key, amount)
    crowded, common = shares(amount, rows * top, limit, slope, True), shares(amount, rows * top, limit, slope, False)
    places = jnp.arange(amount)

    def named(tallies, offset_by):
        used = int((tallies > 0).sum())
        fixed = max(1, used // 4)
        moved = fixed + (places - fixed + offset_by * (used - fixed)) % max(1, amount - fixed)
        return jnp.zeros((amount,), jnp.int32).at[sequence[jnp.where(places < fixed, places, moved)]].set(jnp.asarray(tallies, jnp.int32))

    tallies = jnp.where(number % 4 == 0, named(crowded, number // 4), named(common, number - number // 4 - 1))
    mixed = jax.random.permutation(jax.random.fold_in(own, 3), amount)
    giver, taker = mixed[0:amount // 2 * 2:2], mixed[1:amount // 2 * 2:2]
    slack = jnp.minimum(tallies[giver] - 1, limit - tallies[taker]) // 2
    slack = jnp.where((giver == sequence[0]) | (taker == sequence[0]) | (tallies[taker] == 0), 0, jnp.maximum(slack, 0))
    moved = jax.random.randint(jax.random.fold_in(own, 4), (amount // 2,), 0, 1 << 20) % (slack + 1)
    tallies = tallies.at[giver].add(-moved).at[taker].add(moved)
    labels = jnp.searchsorted(jnp.cumsum(tallies), jnp.arange(rows * top), side="right").astype(jnp.int32)
    listing = labels.reshape(top, rows).T
    listing = listing[jax.random.permutation(jax.random.fold_in(own, 1), rows)]
    offset_by = jax.random.randint(jax.random.fold_in(own, 2), (rows, 1), 0, top)
    return jnp.take_along_axis(listing, (jnp.arange(top)[None, :] + offset_by) % top, axis=1)


def shares(count, total, bound, slope, full):
    loads = [(1 << 20) // math.isqrt(grade ** slope) + 1 for grade in range(1, count + 1)]
    largest = bound if full else min(bound, max(-(-total // count), total * loads[0] // sum(loads)))
    least = 1 if total - largest >= count - 1 else 0
    counts, surplus = [largest] + [least] * (count - 1), total - largest - least * (count - 1)
    while surplus > 0:
        candidates = [i for i in range(1, count) if counts[i] < largest] or [i for i in range(1, count) if counts[i] < bound]
        whole, left = sum([loads[i] for i in candidates]), surplus
        for i in candidates:
            more = min(bound - counts[i], max(1, left * loads[i] // whole), surplus)
            counts[i] = counts[i] + more
            surplus = surplus - more
    return np.array(counts)


def centred(own_key, dims, spread, reach, pieces=(), kind=jnp.bfloat16):
    entries = spread * jax.random.normal(own_key, dims, jnp.float32)
    if pieces:
        entries = entries * shard_levels(own_key, dims, pieces, -0.22, 0.18)
    return jnp.clip(entries, -reach, reach).astype(kind)


def setup_inputs(seed: int = 0) -> dict:
    splits = jax.random.split(jax.random.key(seed), 11)
    tokens = centred(splits[0], (TOKENS, D), 1.0, 6.0, ((0, 16),))
    expert_ids_keys = jax.random.split(jax.random.fold_in(splits[1], 1), TOKENS // TOK_DEV)
    expert_ids_turns = jax.random.permutation(jax.random.fold_in(splits[1], 3), TOKENS // TOK_DEV)
    expert_ids = jax.vmap(lambda own, number: routed_block(jax.random.fold_in(splits[1], 2), own, number, TOK_DEV, EXPERTS, TOP, CAP, 1))(expert_ids_keys, expert_ids_turns).reshape((TOKENS, TOP))
    route_weight = jnp.clip(jnp.exp(math.log(1.0) - 2.9957323 * jax.random.uniform(splits[2], (TOKENS, TOP), jnp.float32) ** shard_levels(splits[2], (TOKENS, TOP), ((0, 16),), -0.2, 0.2)), 0.05, 1.0)
    norm_gain = jnp.clip(1.0 + 0.18 * jax.random.normal(splits[3], (D,), jnp.float32), 0.1, 1.9)
    expert_gate = centred(splits[4], (EXPERTS, FF, D), D ** -0.5, 0.125, ((0, 2), (1, 8), (2, 2)), jnp.float32)
    expert_up = centred(splits[5], (EXPERTS, FF, D), D ** -0.5, 0.125, ((0, 2), (1, 8), (2, 2)), jnp.float32)
    expert_down = centred(splits[6], (EXPERTS, FF, D), FF ** -0.5, 0.25, ((0, 2), (1, 8), (2, 2)), jnp.float32)
    shared_gate = centred(splits[7], (SHARED, D), D ** -0.5, 0.125, ((0, 8), (1, 2)), jnp.float32)
    shared_up = centred(splits[8], (SHARED, D), D ** -0.5, 0.125, ((0, 8), (1, 2)), jnp.float32)
    shared_down = centred(splits[9], (SHARED, D), SHARED ** -0.5, 0.25, ((0, 8), (1, 2)), jnp.float32)
    return dict(tokens=tokens, expert_ids=expert_ids, route_weight=route_weight, norm_gain=norm_gain, expert_gate=expert_gate, expert_up=expert_up, expert_down=expert_down, shared_gate=shared_gate, shared_up=shared_up, shared_down=shared_down)


route_scale = 2.5
norm_eps = 1e-06

def blocked_product(rows, weight):
    count = rows.shape[0]
    left = rows.astype(jnp.float32).reshape(count, N_TP, D // N_TP)
    right = weight.astype(jnp.float32).reshape(weight.shape[0], N_TP, D // N_TP)
    parts = jnp.einsum('mbd,fbd->bmf', left, right, precision=lax.Precision.HIGHEST).astype(jnp.bfloat16)
    parts = lax.optimization_barrier(parts)
    return lax.optimization_barrier(jnp.sum(parts.astype(jnp.float32), axis=0))

def feed_forward(rows, gate_weight, up_weight):
    gate_pre = blocked_product(rows, gate_weight)
    up_pre = blocked_product(rows, up_weight)
    return (jax.nn.silu(gate_pre) * up_pre).astype(jnp.bfloat16)

def reference(tokens, expert_ids, route_weight, norm_gain, expert_gate, expert_up, expert_down, shared_gate, shared_up, shared_down):
    gate_round = (expert_gate * norm_gain).astype(jnp.bfloat16)
    up_round = (expert_up * norm_gain).astype(jnp.bfloat16)
    down_round = expert_down.astype(jnp.bfloat16)
    shared_gate_round = (shared_gate * norm_gain).astype(jnp.bfloat16)
    shared_up_round = (shared_up * norm_gain).astype(jnp.bfloat16)
    shared_down_round = shared_down.astype(jnp.bfloat16)
    tok_float = tokens.astype(jnp.float32)
    normed = (tok_float * lax.rsqrt(lax.optimization_barrier(jnp.mean(tok_float * tok_float, axis=1, keepdims=True)) + norm_eps)).astype(jnp.bfloat16)
    share = route_weight / lax.optimization_barrier(jnp.sum(route_weight, axis=1, keepdims=True)) * route_scale
    shared_act = feed_forward(normed, shared_gate_round, shared_up_round)
    shared_out = jnp.dot(shared_act, shared_down_round, preferred_element_type=jnp.float32)
    most_rows = EXPERTS * CAP

    def per_expert(total, expert):
        named = expert_ids == expert
        chosen = lax.optimization_barrier(jnp.sum(jnp.where(named, share, jnp.float32(0.0)), axis=1))
        present = jnp.any(named, axis=1)
        index = jnp.nonzero(present, size=most_rows, fill_value=0)[0].astype(jnp.int32)
        live = jnp.arange(most_rows).astype(jnp.int32) < jnp.sum(present.astype(jnp.int32))
        picked = normed[index]
        act = feed_forward(picked, gate_round[expert], up_round[expert])
        out = jnp.dot(act, down_round[expert], preferred_element_type=jnp.float32).astype(jnp.bfloat16)
        scale = jnp.where(live, chosen[index], jnp.float32(0.0))
        return (total.at[index].add(scale[:, None] * out.astype(jnp.float32)), None)
    start_total = jnp.zeros((TOKENS, D), jnp.float32)
    routed, _ = lax.scan(per_expert, start_total, jnp.arange(EXPERTS).astype(jnp.int32))
    mixed = (shared_out + routed).astype(jnp.bfloat16)
    new_gate = gate_round.reshape(N_GR, N_FS, FF, D)
    new_up = up_round.reshape(N_GR, N_FS, FF, D)
    new_down = down_round.reshape(N_GR, N_FS, FF, D)
    return (mixed, new_gate, new_up, new_down, shared_gate_round, shared_up_round, shared_down_round)
```

```python
import functools

import jax
import jax.numpy as jnp
from jax import lax
from jax.experimental import pallas as pl
from jax.experimental.pallas import tpu as pltpu
from jax.sharding import PartitionSpec as P

route_scale = 2.5
norm_eps = 1e-06
vmem_bytes = 67043328


def fold_gain(weight, gain):
    return (weight * gain).astype(jnp.bfloat16)


def silu(v):
    return v / (1.0 + jnp.exp(-v))


def handover(
    dims,
    tok,
    w0,
    w1,
    w2,
    s0,
    s1,
    s2,
    mixed,
    o0,
    o1,
    o2,
    q0,
    q1,
    q2,
    n0,
    n1,
    n2,
    h0,
    h1,
    h2,
    xs,
    pout,
    pin,
    act,
    oz,
    rety,
    ret,
    psh,
    pshin,
    local_sem,
    out_sem,
    tok_send,
    tok_recv,
    w_send,
    w_recv,
    x_send,
    x_recv,
    sh_send,
    sh_recv,
    shx_send,
    shx_recv,
    p_send,
    p_recv,
    a_send,
    a_recv,
    ry_send,
    ry_recv,
    r_send,
    r_recv,
    ps_send,
    ps_recv,
):
    G, S, TP, T, C, H, F, SF, slots, Y = dims
    Z = S // Y
    E = G * S
    SH = SF * S
    NB = S // TP
    NH = NB * T
    gi, si, ti = lax.axis_index("gr"), lax.axis_index("fs"), lax.axis_index("tp")
    zi, yi = si // Y, lax.rem(si, Y)
    w, new, sh, shn = (w0, w1, w2), (n0, n1, n2), (s0, s1, s2), (h0, h1, h2)
    outs, shouts = (o0, o1, o2), (q0, q1, q2)

    def rdma(src, dst, ssem, rsem, dev):
        return pltpu.make_async_remote_copy(
            src_ref=src,
            dst_ref=dst,
            send_sem=ssem,
            recv_sem=rsem,
            device_id=dev,
            device_id_type=pl.DeviceIdType.MESH,
        )

    def rows(start, step, size):
        return pl.ds(pl.multiple_of(start * step, step), size)

    def each(lo, hi, fn):
        def step(i, c):
            fn(i)
            return c

        lax.fori_loop(lo, hi, step, 0)

    def fs_peer(k):
        return lax.rem(si + k, S)

    def fs_from(k):
        return lax.rem(si + S - k, S)

    def gr_peer(k):
        return lax.rem(gi + k, G)

    def tp_peer(k):
        return lax.rem(ti + k, TP)

    barrier = pltpu.get_barrier_semaphore()

    def greet(axis, peer, n):
        each(
            1,
            n,
            lambda k: pl.semaphore_signal(
                barrier,
                inc=1,
                device_id={axis: peer(k)},
                device_id_type=pl.DeviceIdType.MESH,
            ),
        )

    greet("fs", fs_peer, S)
    greet("gr", gr_peer, G)
    greet("tp", tp_peer, TP)
    pl.semaphore_wait(barrier, S + G + TP - 3)

    def w_copy(m, d, s):
        return rdma(
            w[m].at[d], new[m].at[gi, rows(s, F, F)], w_send.at[m, d], w_recv.at[m, s], {"fs": d}
        )

    def spread(block, s, up, down, act_on, own=False):
        src, place, ssem, rsem, after = block
        at = place(s)

        def hop(way, dev):
            act_on(rdma(src if own else at, at, ssem.at[s, way], rsem.at[s], {"fs": dev}))

        if up:
            pl.when(zi < Z - 1)(lambda: hop(0, si + Y))
        if down:
            pl.when(zi > 0)(lambda: hop(1, si - Y))

        def across(k):
            y = lax.rem(yi + k, Y)
            hop(2 + y, zi * Y + y)

        each(1, Y, across)

    def shx_copy(m, s, g, dev):
        at = sh_place(m, s, g)
        return rdma(at, at, shx_send.at[m, s, dev], shx_recv.at[m, s, g], {"gr": dev})

    def arrive(block, s):
        src, place, ssem, rsem, after = block
        rdma(place(s), place(s), ssem.at[s, 0], rsem.at[s], {"fs": fs_peer(1)}).wait_recv()
        if after is not None:
            after(s)

    def start(c):
        c.start()

    def sent(c):
        c.wait_send()

    def relay(block, step, act_on=start):
        def from_below():
            s = si - step * Y
            if act_on is start:
                arrive(block, s)
            spread(block, s, True, False, act_on)

        def from_above():
            s = si + step * Y
            if act_on is start:
                arrive(block, s)
            spread(block, s, False, True, act_on)

        pl.when(zi >= step)(from_below)
        pl.when(zi + step < Z)(from_above)

    def others_arrive(block, step):
        def at(z):
            each(1, Y, lambda k: arrive(block, z * Y + lax.rem(yi + k, Y)))

        if step == 0:
            at(zi)
        else:
            pl.when(zi >= step)(lambda: at(zi - step))
            pl.when(zi + step < Z)(lambda: at(zi + step))

    def block_sent(block):
        spread(block, si, True, True, sent, own=True)
        for step in range(1, Z):
            relay(block, step, sent)

    def sh_place(m, s, g):
        return shn[m].at[rows(s, SF, SF), rows(g, C // G, C // G)]

    def sh_block(m):
        return (
            sh[m].at[:, rows(gi, C // G, C // G)],
            lambda s: sh_place(m, s, gi),
            sh_send.at[m],
            sh_recv.at[m],
            lambda s: each(1, G, lambda j: shx_copy(m, s, gi, gr_peer(j)).start()),
        )

    tok_block = (tok, lambda s: xs.at[rows(s, T, T)], tok_send, tok_recv, None)
    sh_blocks = [sh_block(m) for m in range(3)]

    def shared_step(step):
        for block in sh_blocks:
            if step < Z:
                relay(block, step)
            others_arrive(block, step - 1)

    def x_copy(m, s, g, dev, own=False):
        place = new[m].at[g, rows(s, F, F)]
        src = w[m].at[s] if own else place
        return rdma(src, place, x_send.at[m, s, dev], x_recv.at[m, s, g], {"gr": dev})

    def local_copies():
        return (
            [pltpu.make_async_copy(w[m].at[si], new[m].at[gi, rows(si, F, F)], local_sem.at[m]) for m in range(3)]
            + [pltpu.make_async_copy(sh[m], shn[m].at[rows(si, SF, SF)], local_sem.at[3 + m]) for m in range(3)]
            + [pltpu.make_async_copy(tok, xs.at[rows(si, T, T)], local_sem.at[6])]
        )

    def send_weight(m):
        each(1, S, lambda k: w_copy(m, fs_peer(k), si).start())

    for m in range(3):
        each(1, G, lambda j, m=m: x_copy(m, si, gi, gr_peer(j), own=True).start())
    spread(tok_block, si, True, True, start, own=True)
    send_weight(0)
    for copy in local_copies():
        copy.start()

    def forward(m, lo=1, hi=S):
        def one(k):
            s = fs_from(k)
            w_copy(m, s, s).wait_recv()
            each(1, G, lambda j: x_copy(m, s, gi, gr_peer(j)).start())

        each(lo, hi, one)

    def x_arrive(m, g):
        each(0, S, lambda s: x_copy(m, s, g, g).wait_recv())

    def p_copy(j, t, s):
        return rdma(
            pout.at[j if slots > 1 else 0, t], pin.at[j, s], p_send.at[j, t], p_recv.at[j, s], {"tp": t}
        )

    def a_copy(j, t, s):
        place = act.at[j, rows(s, NH, NH)]
        return rdma(place, place, a_send.at[j, t], a_recv.at[j, s], {"tp": t})

    def first_matmuls(j):
        g = gr_peer(j)
        slot = j if slots > 1 else 0
        for q in range(TP):
            t = tp_peer(1 + q)

            def block(b, t=t):
                x = xs[rows(t * NB + b, T, T), 0:C]
                for m in range(2):
                    part = lax.dot_general(
                        x, new[m][g], (((1,), (1,)), ((), ())), preferred_element_type=jnp.float32
                    )
                    pout[slot, t, rows(b, T, T), m * H : (m + 1) * H] = part.astype(jnp.bfloat16)

            each(0, NB, block)
            if q < TP - 1:
                p_copy(j, t, ti).start()

    def activations(j):
        g = gr_peer(j)
        slot = j if slots > 1 else 0
        expert = g * S + si
        for q in range(1, TP):
            t = tp_peer(q)
            p_copy(j, t, t).wait_recv()

        def block(b):
            r = rows(b, T, T)
            pre = pout[slot, ti, r, :].astype(jnp.float32)
            for q in range(1, TP):
                pre = pre + pin[j, tp_peer(q), r, :].astype(jnp.float32)
            at = rows(ti * NB + b, T, T)
            coded = xs[at, C:].astype(jnp.float32)
            lane = lax.broadcasted_iota(jnp.int32, coded.shape, 1)
            share = jnp.sum(
                jnp.where((lane == expert) | (lane == expert + E), coded, 0.0), axis=1, keepdims=True
            )
            value = silu(pre[:, :H]) * pre[:, H:] * share
            act[j, at, :] = value.astype(jnp.bfloat16)

        each(0, NB, block)
        for q in range(1, TP):
            a_copy(j, tp_peer(q), ti).start()

    if Z > 1:
        relay(tok_block, 1)
    send_weight(1)
    forward(0)
    for step in range(2, Z):
        relay(tok_block, step)
    send_weight(2)
    for block in sh_blocks:
        spread(block, si, True, True, start, own=True)
    forward(1)
    for copy in local_copies():
        copy.wait()
    for step in range(Z):
        others_arrive(tok_block, step)
    for j in range(G):
        if j > 0:
            for m in range(2):
                x_arrive(m, gr_peer(j))
            if slots == 1:
                for q in range(1, TP):
                    p_copy(j - 1, tp_peer(q), ti).wait_send()
        first_matmuls(j)
        if j == 1:
            forward(2, S // 2, S)
        activations(j)
        if j == 0:
            forward(2, 1, S // 2 if G > 1 else S)
    shared_step(1)

    for m in range(2):
        pltpu.make_async_copy(new[m], outs[m], out_sem.at[m]).start()
    for j in range(1, G):
        x_arrive(2, gr_peer(j))
    pltpu.make_async_copy(new[2], outs[2], out_sem.at[2]).start()

    def ry_copy(z, y, src):
        return rdma(
            oz.at[rows(z * Y + y, T, T)],
            rety.at[z, src],
            ry_send.at[z, y],
            ry_recv.at[z, src],
            {"fs": zi * Y + y},
        )

    def r_copy(z, up, dist):
        slot = Z if dist == 1 and not up else z
        return rdma(
            oz.at[rows(z * Y + yi, T, T)],
            ret.at[slot],
            r_send.at[z],
            r_recv.at[slot],
            {"fs": si + Y if up else si - Y},
        )

    def far_first(fn):
        for dist in range(Z - 1, -1, -1):
            pl.when(zi + dist < Z)(functools.partial(fn, zi + dist, True, dist))
            if dist:
                pl.when(zi >= dist)(functools.partial(fn, zi - dist, False, dist))

    for q in range(1, TP):
        for j in range(G):
            a_copy(j, tp_peer(q), tp_peer(q)).wait_recv()

    def down_block(z, up, dist):
        def column(k):
            y = lax.rem(yi + k, Y)
            at = rows(z * Y + y, T, T)
            total = jnp.zeros((T, C), jnp.float32)
            for j in range(G):
                total = total + jnp.dot(
                    act[j, at, :], new[2][gr_peer(j)], preferred_element_type=jnp.float32
                )
            oz[at, :] = total.astype(jnp.bfloat16)
            pl.when(y != yi)(lambda: ry_copy(z, y, yi).start())

        each(1, Y + 1, column)

    far_first(down_block)
    if Z > 1:
        shared_step(2)

    def add_far(z, slot):
        at = rows(z * Y + yi, T, T)
        rdma(
            ret.at[slot], ret.at[slot], r_send.at[z], r_recv.at[slot], {"fs": fs_peer(1)}
        ).wait_recv()
        total = oz[at, :].astype(jnp.float32) + ret[slot].astype(jnp.float32)
        oz[at, :] = total.astype(jnp.bfloat16)

    def column_sum(z, up, dist):
        at = rows(z * Y + yi, T, T)
        total = oz[at, :].astype(jnp.float32)
        for k in range(1, Y):
            y = lax.rem(yi + k, Y)
            ry_copy(z, y, y).wait_recv()
            total = total + rety[z, y].astype(jnp.float32)
        oz[at, :] = total.astype(jnp.bfloat16)
        if dist == 0 or up:
            pl.when(zi > 0)(lambda: add_far(z, z))
        if dist == 0:
            pl.when(zi < Z - 1)(lambda: add_far(z, Z))
        elif not up:
            pl.when(zi < Z - 1)(lambda: add_far(z, z))
        if dist:
            r_copy(z, up, dist).start()

    far_first(column_sum)
    for step in range(3, Z + 1):
        shared_step(step)

    def shared_arrive(m):
        each(
            1,
            S,
            lambda k: each(
                1, G, lambda j: shx_copy(m, fs_from(k), gr_peer(j), gr_peer(j)).wait_recv()
            ),
        )

    def ps_copy(t, s):
        return rdma(psh, pshin.at[s], ps_send.at[t], ps_recv.at[s], {"tp": t})

    for m in range(2):
        shared_arrive(m)
        part = lax.dot_general(
            xs[rows(si, T, T), 0:C],
            shn[m][...],
            (((1,), (1,)), ((), ())),
            preferred_element_type=jnp.float32,
        )
        psh[:, m * SH : (m + 1) * SH] = part.astype(jnp.bfloat16)
        pltpu.make_async_copy(shn[m], shouts[m], out_sem.at[3 + m]).start()
    for q in range(1, TP):
        ps_copy(tp_peer(q), ti).start()
    shared_arrive(2)
    pltpu.make_async_copy(shn[2], shouts[2], out_sem.at[5]).start()
    pre = psh[...].astype(jnp.float32)
    for q in range(1, TP):
        t = tp_peer(q)
        ps_copy(t, t).wait_recv()
        pre = pre + pshin[t].astype(jnp.float32)
    shared_act = (silu(pre[:, :SH]) * pre[:, SH:]).astype(jnp.bfloat16)
    total = jnp.dot(shared_act, shn[2][...], preferred_element_type=jnp.float32)
    total = total + oz[rows(si, T, T), :].astype(jnp.float32)
    mixed[...] = total.astype(jnp.bfloat16)

    for m in range(3):
        pltpu.make_async_copy(new[m], outs[m], out_sem.at[m]).wait()
        pltpu.make_async_copy(shn[m], shouts[m], out_sem.at[3 + m]).wait()
        each(1, S, lambda k, m=m: w_copy(m, fs_peer(k), si).wait_send())
        block_sent(sh_blocks[m])
        each(
            1,
            S,
            lambda k, m=m: each(
                1, G, lambda j: shx_copy(m, fs_from(k), gi, gr_peer(j)).wait_send()
            ),
        )
        each(0, S, lambda s, m=m: each(1, G, lambda j: x_copy(m, s, gi, gr_peer(j)).wait_send()))
    block_sent(tok_block)
    each(0, Z, lambda z: each(1, Y, lambda k: ry_copy(z, lax.rem(yi + k, Y), yi).wait_send()))

    def r_sent(z, up, dist):
        if dist:
            r_copy(z, up, dist).wait_send()

    far_first(r_sent)
    for q in range(1, TP):
        t = tp_peer(q)
        ps_copy(t, ti).wait_send()
        for j in range(G):
            if slots > 1 or j == G - 1:
                p_copy(j, t, ti).wait_send()
            a_copy(j, t, ti).wait_send()


def body(
    Y,
    tokens,
    expert_ids,
    route_weight,
    norm_gain,
    expert_gate,
    expert_up,
    expert_down,
    shared_gate,
    shared_up,
    shared_down,
):
    G, S, TP = lax.axis_size("gr"), lax.axis_size("fs"), lax.axis_size("tp")
    T, C = tokens.shape[0], expert_gate.shape[2]
    F, SF = expert_gate.shape[1], shared_gate.shape[0]
    H, SH = F * S, SF * S
    E, N = G * S, S * T
    NH = N // TP
    lanes = -(-2 * E // 128) * 128
    bf16 = jnp.bfloat16

    tok_float = tokens.astype(jnp.float32)
    normed = (
        tok_float * lax.rsqrt(jnp.mean(tok_float * tok_float, axis=1, keepdims=True) + norm_eps)
    ).astype(bf16)
    normed_cols = lax.dynamic_slice_in_dim(normed, lax.axis_index("tp") * C, C, 1)
    share = route_weight / jnp.sum(route_weight, axis=1, keepdims=True) * route_scale
    lane = jnp.arange(lanes, dtype=jnp.int32)[None, None, :]
    dense = jnp.sum(
        jnp.where(expert_ids[:, :, None] == lane % E, share[:, :, None], 0.0), axis=1
    )
    high = dense.astype(bf16)
    low = (dense - lax.reduce_precision(dense, 8, 7)).astype(bf16)
    place = lane[0]
    coded = jnp.where(place < E, high, jnp.where(place < 2 * E, low, 0))
    payload = jnp.concatenate([normed_cols, coded.astype(bf16)], axis=1)

    weights = (
        fold_gain(expert_gate, norm_gain),
        fold_gain(expert_up, norm_gain),
        expert_down.astype(bf16),
    )
    shared = (
        fold_gain(shared_gate, norm_gain),
        fold_gain(shared_up, norm_gain),
        shared_down.astype(bf16),
    )
    row_bytes = 2 * (2 * G * 2 * H + G * H + 3 * C + lanes)
    slots = G if N * row_bytes < vmem_bytes * 3 // 5 else 1
    dims = (G, S, TP, T, C, H, F, SF, slots, Y)
    vmem, hbm = pl.BlockSpec(memory_space=pltpu.VMEM), pl.BlockSpec(memory_space=pl.ANY)
    dma = pltpu.SemaphoreType.DMA
    results = pl.pallas_call(
        functools.partial(handover, dims),
        out_shape=[jax.ShapeDtypeStruct((T, C), bf16)]
        + [jax.ShapeDtypeStruct((G, H, C), bf16)] * 3
        + [jax.ShapeDtypeStruct((SH, C), bf16)] * 3,
        in_specs=[vmem] * 7,
        out_specs=[vmem] + [hbm] * 6,
        scratch_shapes=[pltpu.VMEM((G, H, C), bf16)] * 3
        + [pltpu.VMEM((SH, C), bf16)] * 3
        + [
            pltpu.VMEM((N, C + lanes), bf16),
            pltpu.VMEM((slots, TP, NH, 2 * H), bf16),
            pltpu.VMEM((G, TP, NH, 2 * H), bf16),
            pltpu.VMEM((G, N, H), bf16),
            pltpu.VMEM((N, C), bf16),
            pltpu.VMEM((S // Y, Y, T, C), bf16),
            pltpu.VMEM((S // Y + 1, T, C), bf16),
            pltpu.VMEM((T, 2 * SH), bf16),
            pltpu.VMEM((TP, T, 2 * SH), bf16),
            dma((7,)),
            dma((6,)),
            dma((S, 2 + Y)),
            dma((S,)),
            dma((3, S)),
            dma((3, S)),
            dma((3, S, G)),
            dma((3, S, G)),
            dma((3, S, 2 + Y)),
            dma((3, S)),
            dma((3, S, G)),
            dma((3, S, G)),
            dma((G, TP)),
            dma((G, TP)),
            dma((G, TP)),
            dma((G, TP)),
            dma((S // Y, Y)),
            dma((S // Y, Y)),
            dma((S // Y,)),
            dma((S // Y + 1,)),
            dma((TP,)),
            dma((TP,)),
        ],
        compiler_params=pltpu.CompilerParams(
            collective_id=0, has_side_effects=True, vmem_limit_bytes=vmem_bytes
        ),
        name="handover",
    )(payload, *weights, *shared)
    mixed = results[0]
    whole = [r.reshape(G, 1, H, C) for r in results[1:4]]
    return (mixed, *whole, *results[4:])


def line_length(mesh):
    places = [d.coords for d in mesh.devices[0, :, 0]]
    axis = [i for i in range(3) if places[0][i] != places[1][i]][0]
    count = 0
    for place in places:
        if any(place[i] != places[0][i] for i in range(3) if i != axis):
            break
        count += 1
    return count if len(places) % count == 0 else len(places)


def solution(mesh):
    placed = (
        P(("gr", "fs"), None),
        P(("gr", "fs"), None),
        P(("gr", "fs"), None),
        P("tp"),
        P("gr", "fs", "tp"),
        P("gr", "fs", "tp"),
        P("gr", "fs", "tp"),
        P("fs", "tp"),
        P("fs", "tp"),
        P("fs", "tp"),
    )
    return jax.shard_map(
        functools.partial(body, line_length(mesh)),
        mesh=mesh,
        in_specs=placed,
        out_specs=(
            P(("gr", "fs"), "tp"),
            P(None, "fs", None, "tp"),
            P(None, "fs", None, "tp"),
            P(None, "fs", None, "tp"),
            P(None, "tp"),
            P(None, "tp"),
            P(None, "tp"),
        ),
        check_vma=False,
    )
```
